512 devices in a mesh: sp: 64 (over z, y), tp: 8 (over x, core).
Axes of the slice: x: 4, y: 4, z: 16, core: 2. Of those that a mesh axis runs over, the one named last changes fastest.
Arguments:
- asking_matrix: bfloat16 [8192, 2048], P('sp', 'tp'), may hold values from -30 to 30
- matching_key_matrix: bfloat16 [8192, 1024], P('sp', 'tp'), may hold values from -30 to 30
- carried_value_matrix: bfloat16 [8192, 1024], P('sp', 'tp'), may hold values from -48 to 48
- silu_switch_argument: bfloat16 [8192, 2048], P('sp', 'tp'), may hold values from -6 to 6
- duality_source_matrix: bfloat16 [8192, 2048], P('sp', 'tp'), may hold values from -6 to 6
- storing_direction_matrix: bfloat16 [8192, 1024], P('sp', 'tp'), may hold values from -6 to 6
- fetching_direction_matrix: bfloat16 [8192, 1024], P('sp', 'tp'), may hold values from -6 to 6
- duality_kernel_coefficients: bfloat16 [5, 2048], P(None, 'tp'), may hold values from -2.5 to 2.5
- storing_kernel_coefficients: bfloat16 [5, 1024], P(None, 'tp'), may hold values from -2.5 to 2.5
- fetching_kernel_coefficients: bfloat16 [5, 1024], P(None, 'tp'), may hold values from -2.5 to 2.5
- raw_increment_lengths: float32 [2, 32, 8192], P(None, 'tp', 'sp'), may hold values from -5.5 to 5.5
- logarithmic_fading_speeds: float32 [2, 32], P(None, 'tp'), may hold values from -16 to -2.9
- token_fading_spikes: float32 [2, 32, 8192], P(None, 'tp', 'sp'), may hold values from -2.1 to 0
- absorber_score_vector: float32 [16], P('tp'), may hold values from 4 to 8
- cluster_scaling_factor: float32 [2048], P('tp'), may hold values from 0.1 to 1.9
- final_mapping_matrix: bfloat16 [2, 2048, 4096], P(None, 'tp', 'sp'), may hold values from -0.09375 to 0.09375
Outputs:
- mixed_out: bfloat16 [8192, 4096], P(('sp', 'tp'))
The draws below stay inside these ranges and needn't reach their ends.
All inputs are finite; a program needn't handle non-finite values.
Results may differ from the reference program's by a relative error of at most 0.014.
Values may be sent and summed in bfloat16 or wider, within the bound.
A program may use at most 64 MiB of HBM per device.

```python
import math
import jax
import jax.numpy as jnp
from jax import lax

D = 4096
HEADS = 16
KV_HEADS = 8
HEAD = 128
SSD_HEADS = 32
SSD_HEAD = 64
GROUPS = 8
STATE = 128
CONV = 5
WINDOW = 128
SPAN = 128
TOK_DEV = 128
TOKENS = 8192
ATTN_W = 2048
KV_W = 1024
SSD_W = 2048
N_TP = 8


def drawn_rows(key):
    query_base = jnp.clip(jax.random.normal(jax.random.fold_in(key, 11), (TOKENS, ATTN_W), jnp.float32), -4.0, 4.0)
    key_base = jnp.clip(jax.random.normal(jax.random.fold_in(key, 12), (TOKENS, KV_W), jnp.float32), -4.0, 4.0)
    return (query_base, key_base)


def draw_asking_matrix(key, part):
    return drawn_rows(key)[0].astype(jnp.bfloat16)


def draw_matching_key_matrix(key, part):
    return drawn_rows(key)[1].astype(jnp.bfloat16)


def draw_raw_increment_lengths(key, part):
    jitter = jnp.clip(jax.random.normal(jax.random.fold_in(key, 21), (2, SSD_HEADS, TOKENS), jnp.float32), -4.0, 4.0)
    block_level = jax.random.uniform(jax.random.fold_in(key, 22), (2, SSD_HEADS, TOKENS // TOK_DEV), jnp.float32, -1.5, 1.5)
    return jitter + jnp.repeat(block_level, TOK_DEV, axis=2)


def draw_logarithmic_fading_speeds(key, part):
    keep_count = SSD_HEADS // 2
    ranking = jnp.stack([jax.random.permutation(jax.random.fold_in(key, 31), SSD_HEADS), jax.random.permutation(jax.random.fold_in(key, 32), SSD_HEADS)])
    lasting = ranking < keep_count
    slow_rate = jnp.exp(jax.random.uniform(jax.random.fold_in(key, 33), (2, SSD_HEADS), jnp.float32, math.log(0.02), math.log(0.3))) / TOKENS
    fast_rate = jnp.exp(jax.random.uniform(jax.random.fold_in(key, 34), (2, SSD_HEADS), jnp.float32, math.log(1.0 / 70.0), math.log(1.0 / 20.0)))
    return jnp.log(jnp.where(lasting, slow_rate, fast_rate))


def draw_token_fading_spikes(key, part):
    positions = jax.random.randint(jax.random.fold_in(key, 41), (2, SSD_HEADS, 3), 0, TOKENS)
    depths = jax.random.uniform(jax.random.fold_in(key, 42), (2, SSD_HEADS, 3), jnp.float32, 0.22, 0.69)
    places = jnp.arange(TOKENS, dtype=jnp.int32)
    hits = jnp.where(places[None, None, None, :] == positions[..., None], depths[..., None], 0.0)
    return -jnp.sum(hits, axis=2)


def block_levels(rng, dims, shards, smallest, top_value):
    loudness, own = 1.0, jax.random.fold_in(rng, 6)
    for position, blocks in shards:
        heights = jnp.exp(jax.random.uniform(jax.random.fold_in(own, position), (blocks,), jnp.float32, smallest / len(shards), top_value / len(shards)))
        loudness = loudness * jnp.repeat(heights, dims[position] // blocks).reshape([-1 if axis == position else 1 for axis in range(len(dims))])
    return loudness


def noise(stream_key, shape, scale, most, split=(), held_as=jnp.bfloat16):
    gain = block_levels(stream_key, shape, split, -0.22, 0.18) if split else 1.0
    values = jax.random.normal(stream_key, shape, jnp.float32) * scale * gain
    return jnp.minimum(jnp.maximum(values, -most), most).astype(held_as)


def setup_inputs(seed: int = 0) -> dict:
    key_of = jax.random.split(jax.random.key(seed), 17)
    asking_matrix = draw_asking_matrix(jax.random.fold_in(key_of[16], 71), 0)
    matching_key_matrix = draw_matching_key_matrix(jax.random.fold_in(key_of[16], 71), 0)
    carried_value_matrix = noise(key_of[2], (TOKENS, KV_W), 8.0, 48.0, ((0, 64), (1, 8)))
    silu_switch_argument = noise(key_of[3], (TOKENS, SSD_W), 1.0, 6.0, ((0, 64), (1, 8)))
    duality_source_matrix = noise(key_of[4], (TOKENS, SSD_W), 1.0, 6.0, ((0, 64), (1, 8)))
    storing_direction_matrix = noise(key_of[5], (TOKENS, GROUPS * STATE), 1.0, 6.0, ((0, 64), (1, 8)))
    fetching_direction_matrix = noise(key_of[6], (TOKENS, GROUPS * STATE), 1.0, 6.0, ((0, 64), (1, 8)))
    duality_kernel_coefficients = noise(key_of[7], (CONV, SSD_W), CONV ** -0.5, 2.5, ((1, 8),))
    storing_kernel_coefficients = noise(key_of[8], (CONV, GROUPS * STATE), CONV ** -0.5, 2.5, ((1, 8),))
    fetching_kernel_coefficients = noise(key_of[9], (CONV, GROUPS * STATE), CONV ** -0.5, 2.5, ((1, 8),))
    raw_increment_lengths = draw_raw_increment_lengths(jax.random.fold_in(key_of[16], 71), 0)
    logarithmic_fading_speeds = draw_logarithmic_fading_speeds(jax.random.fold_in(key_of[16], 71), 0)
    token_fading_spikes = draw_token_fading_spikes(jax.random.fold_in(key_of[16], 71), 0)
    absorber_score_vector = jnp.clip(4.0 + 4.0 * jax.random.uniform(key_of[13], (HEADS,), jnp.float32) ** block_levels(key_of[13], (HEADS,), ((0, 8),), -0.2, 0.2), 4.0, 8.0)
    cluster_scaling_factor = jnp.clip(1.0 + 0.18 * jax.random.normal(key_of[14], (SSD_W,), jnp.float32), 0.1, 1.9)
    final_mapping_matrix = noise(key_of[15], (2, ATTN_W, D), (2 * ATTN_W) ** -0.5, 0.09375, ((1, 8), (2, 64)))
    return {"asking_matrix": asking_matrix, "matching_key_matrix": matching_key_matrix, "carried_value_matrix": carried_value_matrix, "silu_switch_argument": silu_switch_argument, "duality_source_matrix": duality_source_matrix, "storing_direction_matrix": storing_direction_matrix, "fetching_direction_matrix": fetching_direction_matrix, "duality_kernel_coefficients": duality_kernel_coefficients, "storing_kernel_coefficients": storing_kernel_coefficients, "fetching_kernel_coefficients": fetching_kernel_coefficients, "raw_increment_lengths": raw_increment_lengths, "logarithmic_fading_speeds": logarithmic_fading_speeds, "token_fading_spikes": token_fading_spikes, "absorber_score_vector": absorber_score_vector, "cluster_scaling_factor": cluster_scaling_factor, "final_mapping_matrix": final_mapping_matrix}


ROTARY_BASE = 500000.0
EPSILON = 1e-06

def rotate(matrix, offset):
    row_count = matrix.shape[0]
    halfway = HEAD // 2
    heads_here = matrix.shape[1] // HEAD
    spacing = ROTARY_BASE ** (-jnp.arange(halfway, dtype=jnp.float32) * 2.0 / HEAD)
    places = (offset + jnp.arange(row_count, dtype=jnp.int32)).astype(jnp.float32)
    angles = places[:, None] * spacing[None, :]
    cosine = jnp.cos(angles)[:, None, :]
    sine_table = jnp.sin(angles)[:, None, :]
    halves = matrix.astype(jnp.float32).reshape(row_count, heads_here, 2, halfway)
    former = halves[:, :, 0]
    latter = halves[:, :, 1]
    turned = jnp.stack([former * cosine - latter * sine_table, latter * cosine + former * sine_table], axis=2)
    return turned.reshape(row_count, heads_here * HEAD).astype(jnp.bfloat16)

def attend(turned_queries, turned_keys, carried_value_matrix, absorber_score_vector):
    sharing = HEADS // KV_HEADS
    block_count = TOKENS // SPAN
    filler = jnp.zeros((SPAN, KV_W), jnp.bfloat16)
    key_pad = jnp.concatenate([filler, turned_keys, filler], axis=0)
    value_pad = jnp.concatenate([filler, carried_value_matrix, filler], axis=0)
    within = jnp.arange(SPAN, dtype=jnp.int32)[:, None]
    across = jnp.arange(3 * SPAN, dtype=jnp.int32)[None, :]
    inside = jnp.abs(across - SPAN - within) <= WINDOW
    sink_rows = absorber_score_vector.reshape(KV_HEADS, sharing)[:, :, None, None]

    def one_block(block_index):
        first_row = (block_index * SPAN).astype(jnp.int32)
        query_tile = lax.dynamic_slice_in_dim(turned_queries, first_row, SPAN, 0).reshape(SPAN, KV_HEADS, sharing, HEAD)
        key_tile = lax.dynamic_slice_in_dim(key_pad, first_row, 3 * SPAN, 0).reshape(3 * SPAN, KV_HEADS, HEAD)
        value_tile = lax.dynamic_slice_in_dim(value_pad, first_row, 3 * SPAN, 0).reshape(3 * SPAN, KV_HEADS, HEAD)
        places = first_row - SPAN + across
        allowed = inside & (places >= 0) & (places < TOKENS)
        scores = jnp.einsum('qkgd,skd->kgqs', query_tile.astype(jnp.float32), key_tile.astype(jnp.float32)) * HEAD ** (-0.5)
        scores = jnp.where(allowed, scores, -jnp.inf)
        ceiling = jnp.maximum(lax.optimization_barrier(jnp.max(scores, axis=-1, keepdims=True)), sink_rows)
        weights = jnp.exp(scores - ceiling)
        denominator = lax.optimization_barrier(jnp.sum(weights, axis=-1, keepdims=True)) + jnp.exp(sink_rows - ceiling)
        probabilities = (weights / denominator).astype(jnp.bfloat16)
        attended = jnp.einsum('kgqs,skd->qkgd', probabilities.astype(jnp.float32), value_tile.astype(jnp.float32))
        return attended.reshape(SPAN, ATTN_W).astype(jnp.bfloat16)
    return lax.map(one_block, jnp.arange(block_count, dtype=jnp.int32)).reshape(TOKENS, ATTN_W)

def convolve(padded, taps_all, row_count):
    summed = jnp.zeros((row_count, padded.shape[1]), jnp.float32)
    for tap_index in range(CONV):
        summed = summed + padded[tap_index:tap_index + row_count].astype(jnp.float32) * taps_all[tap_index].astype(jnp.float32)
    return jax.nn.silu(summed).astype(jnp.bfloat16)

def sweep(scan_rows, step_rows, decay_rows, write_rows, read_rows):
    per_group = SSD_HEADS // GROUPS
    block_count = TOKENS // SPAN
    highest = lax.Precision.HIGHEST
    scan_tiles = scan_rows.reshape(block_count, SPAN, GROUPS, per_group, SSD_HEAD)
    step_tiles = step_rows.reshape(block_count, SPAN, GROUPS, per_group)
    decay_tiles = decay_rows.reshape(block_count, SPAN, GROUPS, per_group)
    write_tiles = write_rows.reshape(block_count, SPAN, GROUPS, STATE)
    read_tiles = read_rows.reshape(block_count, SPAN, GROUPS, STATE)
    earlier_mask = jnp.arange(SPAN)[:, None] >= jnp.arange(SPAN)[None, :]

    def advance(carried, block_item):
        scan_tile, step_tile, decay_tile, write_tile, read_tile = block_item
        scaled = scan_tile.astype(jnp.float32) * step_tile[..., None]
        write_values = write_tile.astype(jnp.float32)
        read_values = read_tile.astype(jnp.float32)
        running = jnp.cumsum(decay_tile, axis=0)
        spread = running[:, None] - running[None, :]
        fading = jnp.exp(jnp.where(earlier_mask[:, :, None, None], spread, -jnp.inf))
        affinity = jnp.einsum('lgn,sgn->lsg', read_values, write_values, precision=highest)
        within_block = jnp.einsum('lsgr,sgrp->lgrp', affinity[..., None] * fading, scaled, precision=highest)
        from_before = jnp.einsum('lgn,grpn->lgrp', read_values, carried, precision=highest) * jnp.exp(running)[..., None]
        to_end = jnp.exp(running[-1:] - running)
        block_states = jnp.einsum('lgn,lgrp->grpn', write_values, scaled * to_end[..., None], precision=highest)
        return (carried * jnp.exp(running[-1])[..., None, None] + block_states, within_block + from_before)
    start_state = jnp.zeros((GROUPS, per_group, SSD_HEAD, STATE), jnp.float32)
    final_state, outputs = lax.scan(advance, start_state, (scan_tiles, step_tiles, decay_tiles, write_tiles, read_tiles))
    return outputs.reshape(TOKENS, SSD_W)

def reference(asking_matrix, matching_key_matrix, carried_value_matrix, silu_switch_argument, duality_source_matrix, storing_direction_matrix, fetching_direction_matrix, duality_kernel_coefficients, storing_kernel_coefficients, fetching_kernel_coefficients, raw_increment_lengths, logarithmic_fading_speeds, token_fading_spikes, absorber_score_vector, cluster_scaling_factor, final_mapping_matrix):
    attended = attend(rotate(asking_matrix, 0), rotate(matching_key_matrix, 0), carried_value_matrix, absorber_score_vector)
    margin = CONV // 2
    raw_rows = jnp.concatenate([duality_source_matrix, storing_direction_matrix, fetching_direction_matrix], axis=1)
    padded = jnp.pad(raw_rows, ((margin, margin), (0, 0)))
    conved = convolve(padded, jnp.concatenate([duality_kernel_coefficients, storing_kernel_coefficients, fetching_kernel_coefficients], axis=1), TOKENS)
    per_group = SSD_HEADS // GROUPS
    scan_rows = conved[:, :SSD_W].reshape(TOKENS, GROUPS, per_group, SSD_HEAD)
    write_rows = conved[:, SSD_W:SSD_W + GROUPS * STATE].reshape(TOKENS, GROUPS, STATE)
    read_rows = conved[:, SSD_W + GROUPS * STATE:].reshape(TOKENS, GROUPS, STATE)
    joint_increment_lengths = jax.nn.softplus(raw_increment_lengths)
    joint_fading_amounts = -jnp.exp(logarithmic_fading_speeds)[:, :, None] * joint_increment_lengths + token_fading_spikes
    steps_rows = jnp.transpose(joint_increment_lengths, (0, 2, 1)).reshape(2, TOKENS, GROUPS, per_group)
    decay_rows = jnp.transpose(joint_fading_amounts, (0, 2, 1)).reshape(2, TOKENS, GROUPS, per_group)
    ahead_rows = sweep(scan_rows, steps_rows[0], decay_rows[0], write_rows, read_rows)
    back_rows = sweep(scan_rows[::-1], steps_rows[1][::-1], decay_rows[1][::-1], write_rows[::-1], read_rows[::-1])[::-1]
    gated_rows = (ahead_rows + back_rows) * jax.nn.silu(silu_switch_argument.astype(jnp.float32))
    grouped = gated_rows.reshape(TOKENS, GROUPS, SSD_W // GROUPS)
    grouped = grouped * lax.rsqrt(lax.optimization_barrier(jnp.mean(grouped * grouped, axis=-1, keepdims=True)) + EPSILON)
    normed = (grouped.reshape(TOKENS, SSD_W) * cluster_scaling_factor).astype(jnp.bfloat16)
    slice_width = ATTN_W // N_TP
    summed = jnp.zeros((TOKENS, D), jnp.float32)
    for shard_index in range(N_TP):
        first_col = shard_index * slice_width
        partial_sum = jnp.dot(attended[:, first_col:first_col + slice_width], final_mapping_matrix[0, first_col:first_col + slice_width], preferred_element_type=jnp.float32)
        partial_sum = partial_sum + jnp.dot(normed[:, first_col:first_col + slice_width], final_mapping_matrix[1, first_col:first_col + slice_width], preferred_element_type=jnp.float32)
        rounded = lax.optimization_barrier(partial_sum.astype(jnp.bfloat16))
        summed = summed + rounded.astype(jnp.float32)
    return summed.astype(jnp.bfloat16)
```

```python
import functools

import jax
import jax.numpy as jnp
import numpy as np
from jax import lax
from jax.experimental import pallas as pl
from jax.experimental.pallas import tpu as pltpu
from jax.sharding import PartitionSpec as P

HEAD = 128
TOK = 128
CONV = 5
WINDOW = 128
NY = 4
GROUP = 8
F32 = jnp.float32
BF16 = jnp.bfloat16
ROTARY_BASE = 500000.0
EPSILON = 1e-06
HIGHEST = lax.Precision.HIGHEST


def rotary_tables(blocks):
    half = HEAD // 2
    spacing = ROTARY_BASE ** (-np.arange(half, dtype=np.float64) * 2.0 / HEAD)
    spacing = np.concatenate([spacing, spacing])
    starts = (np.arange(blocks + 2, dtype=np.float64) - 1.0)[:, None] * TOK * spacing[None, :]
    inner = np.arange(TOK, dtype=np.float64)[:, None] * spacing[None, :]
    starts = np.stack([np.cos(starts), np.sin(starts)], axis=1).astype(np.float32)
    inner = np.stack([np.cos(inner), np.sin(inner)]).astype(np.float32)
    return starts, inner


def nt(a, b, **kw):
    return lax.dot_general(a, b, (((1,), (1,)), ((), ())), preferred_element_type=F32, **kw)


def kernel(
    nz, nx,
    q_ref, k_ref, v_ref, z_ref, x_ref, b_ref, c_ref, tx_ref, tb_ref, tc_ref,
    raw_ref, spike_ref, speed_ref, sink_ref, gain_ref, w_ref, start_ref, inner_ref,
    o_ref,
    kbuf, vbuf, hx, hb, hc, pad, yw,
    s1, r1, s2, r2, s3, r3, pf, cf, pb, cb,
    wbuf, wcat, act, pbuf, prx, xbuf, xrx, fin, ybuf,
    halo_s, halo_r, w_s, w_r, s1s, s1r, s2s, s2r, s3s, s3r,
    a_s, a_r, d_s, d_r, x_s, x_r, y_s, y_r,
):
    ng = nz * NY // GROUP
    nsp = nz * NY
    sp = lax.axis_index("sp")
    tp = lax.axis_index("tp")
    m, g = lax.rem(sp, GROUP), lax.div(sp, GROUP)
    y, zz = lax.rem(sp, NY), lax.div(sp, NY)
    xx, core = lax.div(tp, 2), lax.rem(tp, 2)

    def at(s, t):
        return (s, t)

    prev = at(lax.rem(sp + nsp - 1, nsp), tp)
    nxt = at(lax.rem(sp + 1, nsp), tp)
    zprev = at(lax.rem(sp + nsp - NY, nsp), tp)
    znext = at(lax.rem(sp + NY, nsp), tp)
    partner = at(sp, tp + 1 - 2 * core)
    group_peer = [at(g * GROUP + lax.rem(m + d, GROUP), tp) for d in range(GROUP)]
    far_peer = [at(lax.rem(g + d, ng) * GROUP + m, tp) for d in range(ng)]
    y_peer = [at(zz * NY + lax.rem(y + d, NY), tp) for d in range(NY)]
    x_peer = [at(sp, lax.rem(xx + d, nx) * 2 + core) for d in range(nx)]

    barrier = pltpu.get_barrier_semaphore()
    greeted = [prev, nxt, zprev, znext, partner] + group_peer[1:] + far_peer[1:] + x_peer[1:]
    for device in greeted:
        pl.semaphore_signal(barrier, inc=1, device_id=device, device_id_type=pl.DeviceIdType.MESH)

    sends = []

    def send(src, dst, ssem, rsem, device):
        copy = pltpu.make_async_remote_copy(
            src_ref=src, dst_ref=dst, send_sem=ssem, recv_sem=rsem,
            device_id=device, device_id_type=pl.DeviceIdType.MESH,
        )
        copy.start()
        sends.append(copy)

    def arrived(dst, ssem, rsem, device):
        pltpu.make_async_remote_copy(
            src_ref=dst, dst_ref=dst, send_sem=ssem, recv_sem=rsem,
            device_id=device, device_id_type=pl.DeviceIdType.MESH,
        ).wait_recv()

    lane = lax.broadcasted_iota(jnp.int32, (TOK, 128), 1)
    sub = lax.broadcasted_iota(jnp.int32, (TOK, 128), 0)
    low = lane < 64
    low1 = low[:1]

    wbuf[zz, :, 0:64] = w_ref[0]
    wbuf[zz, :, 64:128] = w_ref[1]

    row8 = lax.broadcasted_iota(jnp.int32, (8, 128), 0)
    raw = jnp.concatenate([raw_ref[0], raw_ref[1]], axis=0)
    spike = jnp.concatenate([spike_ref[0], spike_ref[1]], axis=0)
    speed = jnp.zeros((8, 128), F32)
    for i in range(8):
        speed = jnp.where(row8 == i, speed_ref[i // 4, i % 4], speed)
    step = jnp.maximum(raw, 0.0) + jnp.log(1.0 + jnp.exp(-jnp.abs(raw)))
    logdecay = -jnp.exp(speed) * step + spike
    upto = (sub <= lane).astype(F32)
    onward = (sub >= lane).astype(F32)
    cum_f = jnp.dot(logdecay, upto, precision=HIGHEST, preferred_element_type=F32)
    cum_b = jnp.dot(logdecay, onward, precision=HIGHEST, preferred_element_type=F32)
    cum = jnp.where(row8 < 4, cum_f, cum_b)
    total = jnp.broadcast_to(jnp.sum(logdecay, axis=1, keepdims=True), (8, 128))
    to_end = step * jnp.exp(total - cum)
    grown = jnp.exp(cum)
    whole = jnp.exp(total)
    columns = jnp.concatenate([cum, to_end, grown, jnp.zeros((104, 128), F32)], axis=0).T

    def spread(first):
        tiles = [
            jnp.where(low, columns[:, first + 2 * i : first + 2 * i + 1], columns[:, first + 2 * i + 1 : first + 2 * i + 2])
            for i in range(2)
        ]
        return jnp.concatenate(tiles, axis=1)

    def spread_row(first):
        tiles = [
            jnp.where(low1, whole[first + 2 * i : first + 2 * i + 1], whole[first + 2 * i + 1 : first + 2 * i + 2])
            for i in range(2)
        ]
        return jnp.concatenate(tiles, axis=1)

    row16 = lax.broadcasted_iota(jnp.int32, (16, 256), 0)

    def split_rows(values):
        rows = jnp.zeros((16, 256), F32)
        at_row = 0
        for value in values:
            rest = value
            for _ in range(3):
                piece = rest.astype(BF16).astype(F32)
                rows = jnp.where(row16 == at_row, piece, rows)
                rest = rest - piece
                at_row += 1
        return rows.astype(BF16)

    decay_rows = split_rows([spread_row(0), spread_row(4)])

    inner_cos, inner_sin = inner_ref[0], inner_ref[1]

    def turn(value, block):
        cosine = start_ref[sp + block, 0:1, :]
        sine = start_ref[sp + block, 1:2, :]
        here_cos = cosine * inner_cos - sine * inner_sin
        here_sin = sine * inner_cos + cosine * inner_sin
        here_sin = jnp.where(low, -here_sin, here_sin)
        value = value.astype(F32)
        return (value * here_cos + pltpu.roll(value, 64, 1) * here_sin).astype(BF16)

    queries = jnp.concatenate([turn(q_ref[:, 0:128], 1), turn(q_ref[:, 128:256], 1)], axis=0)
    pad[8 : 8 + TOK, 0:256] = x_ref[...].astype(F32)
    pad[8 : 8 + TOK, 256:384] = b_ref[...].astype(F32)
    pad[8 : 8 + TOK, 384:512] = c_ref[...].astype(F32)
    r2[g] = jnp.zeros((32, 256), BF16)

    pl.semaphore_wait(barrier, len(greeted))

    for i, (ref, buf) in enumerate([(x_ref, hx), (b_ref, hb), (c_ref, hc)]):
        send(ref.at[TOK - 16 : TOK], buf.at[0], halo_s.at[2 * i], halo_r.at[2 * i], nxt)
        send(ref.at[0:16], buf.at[1], halo_s.at[2 * i + 1], halo_r.at[2 * i + 1], prev)
    right_steps, left_steps = nz // 2, nz - 1 - nz // 2
    send(wbuf.at[zz], wbuf.at[zz], w_s.at[0, 0], w_r.at[0, 1], znext)
    if left_steps:
        send(wbuf.at[zz], wbuf.at[zz], w_s.at[1, 0], w_r.at[1, 1], zprev)
    for i, (ref, buf) in enumerate([(k_ref, kbuf), (v_ref, vbuf)]):
        send(ref, buf.at[0], halo_s.at[6 + 2 * i], halo_r.at[6 + 2 * i], nxt)
        send(ref, buf.at[1], halo_s.at[7 + 2 * i], halo_r.at[7 + 2 * i], prev)

    def relay(s):
        if s <= right_steps:
            piece = lax.rem(zz + nz - s, nz)
            arrived(wbuf.at[piece], w_s.at[0, 0], w_r.at[0, s], zprev)
            if s < right_steps:
                send(wbuf.at[piece], wbuf.at[piece], w_s.at[0, s], w_r.at[0, s + 1], znext)
        if s <= left_steps:
            piece = lax.rem(zz + s, nz)
            arrived(wbuf.at[piece], w_s.at[1, 0], w_r.at[1, s], znext)
            if s < left_steps:
                send(wbuf.at[piece], wbuf.at[piece], w_s.at[1, s], w_r.at[1, s + 1], zprev)

    has_prev, has_next = sp > 0, sp < nsp - 1
    for i, (buf, first, last) in enumerate([(hx, 0, 256), (hb, 256, 384), (hc, 384, 512)]):
        arrived(buf.at[0], halo_s.at[2 * i], halo_r.at[2 * i], prev)
        arrived(buf.at[1], halo_s.at[2 * i + 1], halo_r.at[2 * i + 1], nxt)
        before = buf[0].astype(F32)[8:16]
        after = buf[1].astype(F32)[0:8]
        pad[0:8, first:last] = jnp.where(has_prev, before, 0.0)
        pad[8 + TOK : 16 + TOK, first:last] = jnp.where(has_next, after, 0.0)

    def convolved(first, last, taps_ref):
        taps = taps_ref[...].astype(F32)
        summed = jnp.zeros((TOK, last - first), F32)
        for k in range(CONV):
            summed = summed + pad[6 + k : 6 + k + TOK, first:last] * taps[k : k + 1]
        return (summed / (1.0 + jnp.exp(-summed))).astype(BF16)

    xs = convolved(0, 256, tx_ref)
    writes = convolved(256, 384, tb_ref)
    reads = convolved(384, 512, tc_ref)

    xs32 = xs.astype(F32)
    ends = jnp.concatenate([xs32 * spread(8), xs32 * spread(12)], axis=1).astype(BF16)
    states = lax.dot_general(
        writes, ends, (((0,), (0,)), ((), ())), preferred_element_type=F32
    ).astype(BF16)
    for j in range(GROUP):
        s1[j, 0:16] = states[16 * j : 16 * j + 16, 0:256]
        s1[j, 16:32] = states[16 * j : 16 * j + 16, 256:512]
        s1[j, 32:48] = decay_rows
    for d in range(1, GROUP):
        send(s1.at[lax.rem(m + d, GROUP)], r1.at[m], s1s.at[d], s1r.at[d], group_peer[d])
    r1[m] = s1[m]

    relay(1)

    for i, buf in enumerate([kbuf, vbuf]):
        arrived(buf.at[0], halo_s.at[6 + 2 * i], halo_r.at[6 + 2 * i], prev)
        arrived(buf.at[1], halo_s.at[7 + 2 * i], halo_r.at[7 + 2 * i], nxt)
    keys = jnp.concatenate([turn(kbuf[0], 0), turn(k_ref[...], 1), turn(kbuf[1], 2)], axis=0)
    values = jnp.concatenate([vbuf[0], v_ref[...], vbuf[1]], axis=0)
    scores = nt(queries, keys) * HEAD ** (-0.5)
    i_q = lax.broadcasted_iota(jnp.int32, (2 * TOK, 3 * TOK), 0) & (TOK - 1)
    j_k = lax.broadcasted_iota(jnp.int32, (2 * TOK, 3 * TOK), 1)
    first_key = jnp.where(has_prev, 0, TOK)
    last_key = jnp.where(has_next, 3 * TOK, 2 * TOK)
    allowed = (jnp.abs(j_k - TOK - i_q) <= WINDOW) & (j_k >= first_key) & (j_k < last_key)
    scores = jnp.where(allowed, scores, -1e30)
    head_row = lax.broadcasted_iota(jnp.int32, (2 * TOK, 1), 0)
    sink = jnp.where(head_row < TOK, sink_ref[0], sink_ref[1])
    top = jnp.maximum(jnp.max(scores, axis=1, keepdims=True), sink)
    weights = jnp.exp(scores - top)
    denominator = jnp.sum(weights, axis=1, keepdims=True) + jnp.exp(sink - top)
    probabilities = (weights / denominator).astype(BF16)
    attended = jnp.dot(probabilities, values, preferred_element_type=F32).astype(BF16)
    act[0, 0, :, 0:128] = attended[0:TOK]
    act[0, 0, :, 128:256] = attended[TOK : 2 * TOK]
    for d in (1, 3, 2):
        send(act.at[0, 0], act.at[NY - d, 0], a_s.at[0, d], a_r.at[0, NY - d], y_peer[d])

    relay(2)

    for d in range(1, GROUP):
        arrived(r1.at[lax.rem(m + GROUP - d, GROUP)], s1s.at[d], s1r.at[d], group_peer[d])
    fades = [r1[j, 32:48].astype(F32) for j in range(GROUP)]
    fade_f = [f[0:1] + f[1:2] + f[2:3] for f in fades]
    fade_b = [f[3:4] + f[4:5] + f[5:6] for f in fades]
    run, fade = jnp.zeros((16, 256), F32), jnp.ones((1, 256), F32)
    for j in range(GROUP):
        pf[j] = run
        cf[j] = jnp.broadcast_to(fade, (8, 256))
        run = run * fade_f[j] + r1[j, 0:16].astype(F32)
        fade = fade * fade_f[j]
    s2[0, 0:16] = run.astype(BF16)
    s2[0, 16:32] = split_rows([fade])
    run, fade = jnp.zeros((16, 256), F32), jnp.ones((1, 256), F32)
    for j in reversed(range(GROUP)):
        pb[j] = run
        cb[j] = jnp.broadcast_to(fade, (8, 256))
        run = run * fade_b[j] + r1[j, 16:32].astype(F32)
        fade = fade * fade_b[j]
    s2[1, 0:16] = run.astype(BF16)
    s2[1, 16:32] = split_rows([fade])
    for d in range(1, ng):
        other = lax.rem(g + d, ng)
        way = jnp.where(other > g, 0, 1)
        send(s2.at[way], r2.at[g], s2s.at[d], s2r.at[d], far_peer[d])

    relay(3)

    affinity = nt(reads, writes)
    for h in range(4):
        ahead = columns[:, h : h + 1] - cum[h : h + 1]
        back = columns[:, 4 + h : 5 + h] - cum[4 + h : 5 + h]
        fading = jnp.exp(jnp.where(lane <= sub, ahead, back))
        step_f, step_b = step[h : h + 1], step[4 + h : 5 + h]
        size = jnp.where(lane < sub, step_f, jnp.where(lane > sub, step_b, step_f + step_b))
        mix = (affinity * fading * size).astype(BF16)
        yw[:, 64 * h : 64 * h + 64] = jnp.dot(mix, xs[:, 64 * h : 64 * h + 64], preferred_element_type=F32)

    relay(4)
    relay(5)

    for d in range(1, ng):
        arrived(r2.at[lax.rem(g + ng - d, ng)], s2s.at[d], s2r.at[d], far_peer[d])
    come_f, come_b = jnp.zeros((16, 256), F32), jnp.zeros((16, 256), F32)
    for j in range(ng):
        f = r2[j, 16:32].astype(F32)
        come_f = jnp.where(j < g, come_f * (f[0:1] + f[1:2] + f[2:3]) + r2[j, 0:16].astype(F32), come_f)
    for j in reversed(range(ng)):
        f = r2[j, 16:32].astype(F32)
        come_b = jnp.where(j > g, come_b * (f[0:1] + f[1:2] + f[2:3]) + r2[j, 0:16].astype(F32), come_b)
    for j in range(GROUP):
        s3[j, 0:16] = (come_f * cf[j, 0:1] + pf[j]).astype(BF16)
        s3[j, 16:32] = (come_b * cb[j, 0:1] + pb[j]).astype(BF16)
    for d in range(1, GROUP):
        send(s3.at[lax.rem(m + d, GROUP)], r3.at[m], s3s.at[d], s3r.at[d], group_peer[d])
    r3[m] = s3[m]

    for s in range(6, max(right_steps, left_steps) + 1):
        relay(s)
    for p in range(nz // 2):
        one, two = wbuf[2 * p], wbuf[2 * p + 1]
        wcat[p // 2, 0:256, 128 * (p % 2) : 128 * (p % 2) + 128] = jnp.concatenate([one[:, 0:64], two[:, 0:64]], axis=1)
        wcat[p // 2, 256:512, 128 * (p % 2) : 128 * (p % 2) + 128] = jnp.concatenate([one[:, 64:128], two[:, 64:128]], axis=1)

    for d in range(1, GROUP):
        arrived(r3.at[lax.rem(m + GROUP - d, GROUP)], s3s.at[d], s3r.at[d], group_peer[d])
    in_f = r3[:, 0:16].reshape(128, 256)
    in_b = r3[:, 16:32].reshape(128, 256)
    both = (
        yw[...]
        + jnp.dot(reads, in_f, preferred_element_type=F32) * spread(16)
        + jnp.dot(reads, in_b, preferred_element_type=F32) * spread(20)
    )
    gate = z_ref[...].astype(F32)
    gated = both * (gate / (1.0 + jnp.exp(-gate)))
    mean = jnp.sum(gated * gated, axis=1, keepdims=True) * (1.0 / 256)
    act[0, 1] = (gated * lax.rsqrt(mean + EPSILON) * gain_ref[...]).astype(BF16)
    for d in (1, 3, 2):
        send(act.at[0, 1], act.at[NY - d, 1], a_s.at[1, d], a_r.at[1, NY - d], y_peer[d])

    n_cols = 64 * nz

    def pair_sum(e):
        arrived(prx.at[e], d_s.at[e], d_r.at[e], partner)
        for c in range(nx):
            rows = slice(16 * c, 16 * c + 16)
            xbuf[e, c] = (pbuf[e, core, rows].astype(F32) + prx[e, rows].astype(F32)).astype(BF16)
        for d in range(1, nx):
            send(xbuf.at[e, lax.rem(xx + d, nx)], xrx.at[e, d], x_s.at[e, d], x_r.at[e, d], x_peer[d])

    order = (0, 1, 3, 2)
    for i, e in enumerate(order):
        if e:
            arrived(act.at[e, 0], a_s.at[0, e], a_r.at[0, e], y_peer[e])
            arrived(act.at[e, 1], a_s.at[1, e], a_r.at[1, e], y_peer[e])
        for n in range(nz // 4):
            part = jnp.dot(act[e, 0], wcat[n, 0:256], preferred_element_type=F32)
            part = part + jnp.dot(act[e, 1], wcat[n, 256:512], preferred_element_type=F32)
            part = part.astype(BF16)
            for c in range(nx):
                for k in range(2):
                    pbuf[e, k, 16 * c : 16 * c + 16, 256 * n : 256 * n + 256] = part[
                        32 * c + 16 * k : 32 * c + 16 * k + 16
                    ]
        send(pbuf.at[e, 1 - core], prx.at[e], d_s.at[e], d_r.at[e], partner)
        if i:
            pair_sum(order[i - 1])
    pair_sum(order[-1])

    for e in order:
        done = xbuf[e, xx].astype(F32)
        for d in range(1, nx):
            arrived(xrx.at[e, d], x_s.at[e, d], x_r.at[e, d], x_peer[d])
            done = done + xrx[e, d].astype(F32)
        if e:
            fin[e] = done.astype(BF16)
            send(fin.at[e], ybuf.at[y], y_s.at[e], y_r.at[NY - e], y_peer[e])
        else:
            ybuf[y] = done.astype(BF16)
    for e in (1, 3, 2):
        arrived(ybuf.at[lax.rem(y + e, NY)], y_s.at[e], y_r.at[e], y_peer[e])
    for p in range(nz // 2):
        cells = [ybuf[j, :, 128 * p : 128 * p + 128] for j in range(NY)]
        for half in range(2):
            for pair in range(2):
                first = 256 * (2 * p + half) + 128 * pair
                o_ref[:, first : first + 128] = jnp.concatenate(
                    [cells[2 * pair + i][:, 64 * half : 64 * half + 64] for i in range(2)], axis=1
                )
    for copy in sends:
        copy.wait_send()


def solution(mesh):
    nz = mesh.shape["sp"] // NY
    nx = mesh.shape["tp"] // 2
    starts, inner = rotary_tables(mesh.shape["sp"])

    def local(
        asking, matching, carried, switch, source, storing, fetching,
        duality_taps, storing_taps, fetching_taps, raw, speeds, spikes, sinks, gains, mapping,
    ):
        cols = 64 * nz
        vmem = pl.BlockSpec(memory_space=pltpu.VMEM)
        smem = pl.BlockSpec(memory_space=pltpu.SMEM)
        dma = pltpu.SemaphoreType.DMA
        ng = nz * NY // GROUP
        rings = nz // 2 + 1
        scratch = [
            pltpu.VMEM((2, TOK, 128), BF16), pltpu.VMEM((2, TOK, 128), BF16),
            pltpu.VMEM((2, 16, 256), BF16), pltpu.VMEM((2, 16, 128), BF16), pltpu.VMEM((2, 16, 128), BF16),
            pltpu.VMEM((TOK + 16, 512), F32), pltpu.VMEM((TOK, 256), F32),
            pltpu.VMEM((GROUP, 48, 256), BF16), pltpu.VMEM((GROUP, 48, 256), BF16),
            pltpu.VMEM((2, 32, 256), BF16), pltpu.VMEM((ng, 32, 256), BF16),
            pltpu.VMEM((GROUP, 32, 256), BF16), pltpu.VMEM((GROUP, 32, 256), BF16),
            pltpu.VMEM((GROUP, 16, 256), F32), pltpu.VMEM((GROUP, 8, 256), F32),
            pltpu.VMEM((GROUP, 16, 256), F32), pltpu.VMEM((GROUP, 8, 256), F32),
            pltpu.VMEM((nz, 256, 128), BF16), pltpu.VMEM((nz // 4, 512, 256), BF16),
            pltpu.VMEM((NY, 2, TOK, 256), BF16),
            pltpu.VMEM((NY, 2, 16 * nx, cols), BF16), pltpu.VMEM((NY, 16 * nx, cols), BF16),
            pltpu.VMEM((NY, nx, 16, cols), BF16), pltpu.VMEM((NY, nx, 16, cols), BF16),
            pltpu.VMEM((NY, 16, cols), BF16), pltpu.VMEM((NY, 16, cols), BF16),
            dma((10,)), dma((10,)), dma((2, rings)), dma((2, rings)),
            dma((GROUP,)), dma((GROUP,)), dma((ng,)), dma((ng,)), dma((GROUP,)), dma((GROUP,)),
            dma((2, NY)), dma((2, NY)), dma((NY,)), dma((NY,)),
            dma((NY, nx)), dma((NY, nx)), dma((NY,)), dma((NY,)),
        ]
        return pl.pallas_call(
            functools.partial(kernel, nz, nx),
            out_shape=jax.ShapeDtypeStruct((TOK // (2 * nx), 4 * cols), BF16),
            in_specs=[vmem] * 12 + [smem, smem] + [vmem] * 4,
            out_specs=vmem,
            scratch_shapes=scratch,
            compiler_params=pltpu.CompilerParams(collective_id=0, has_side_effects=True),
        )(
            asking, matching, carried, switch, source, storing, fetching,
            duality_taps, storing_taps, fetching_taps, raw, spikes, speeds, sinks,
            gains.reshape(1, 256), mapping, jnp.asarray(starts), jnp.asarray(inner),
        )

    return jax.shard_map(
        local,
        mesh=mesh,
        in_specs=(
            P("sp", "tp"), P("sp", "tp"), P("sp", "tp"), P("sp", "tp"), P("sp", "tp"), P("sp", "tp"), P("sp", "tp"),
            P(None, "tp"), P(None, "tp"), P(None, "tp"),
            P(None, "tp", "sp"), P(None, "tp"), P(None, "tp", "sp"), P("tp"), P("tp"), P(None, "tp", "sp"),
        ),
        out_specs=P(("sp", "tp"), None),
        check_vma=False,
    )
```

```python
import functools

import jax
import jax.numpy as jnp
import numpy as np
from jax import lax
from jax.experimental import pallas as pl
from jax.experimental.pallas import tpu as pltpu
from jax.sharding import PartitionSpec as P

HEAD = 128
TOK = 128
CONV = 5
WINDOW = 128
NY = 4
GROUP = 8
F32 = jnp.float32
BF16 = jnp.bfloat16
ROTARY_BASE = 500000.0
EPSILON = 1e-06
HIGHEST = lax.Precision.HIGHEST


def rotary_tables(blocks):
    half = HEAD // 2
    spacing = ROTARY_BASE ** (-np.arange(half, dtype=np.float64) * 2.0 / HEAD)
    spacing = np.concatenate([spacing, spacing])
    starts = (np.arange(blocks + 2, dtype=np.float64) - 1.0)[:, None] * TOK * spacing[None, :]
    inner = np.arange(TOK, dtype=np.float64)[:, None] * spacing[None, :]
    starts = np.stack([np.cos(starts), np.sin(starts)], axis=1).astype(np.float32)
    inner = np.stack([np.cos(inner), np.sin(inner)]).astype(np.float32)
    return starts, inner


def nt(a, b, **kw):
    return lax.dot_general(a, b, (((1,), (1,)), ((), ())), preferred_element_type=F32, **kw)


def kernel(
    nz, nx,
    q_ref, k_ref, v_ref, z_ref, x_ref, b_ref, c_ref, tx_ref, tb_ref, tc_ref,
    raw_ref, spike_ref, speed_ref, sink_ref, gain_ref, w_ref, start_ref, inner_ref,
    o_ref,
    kbuf, vbuf, hx, hb, hc, pad, yw,
    s1, r1, s2, r2, s3, r3, pf, cf, pb, cb,
    wbuf, act, pbuf, prx, xbuf, xrx, fin, ybuf,
    halo_s, halo_r, w_s, w_r, s1s, s1r, s2s, s2r, s3s, s3r,
    a_s, a_r, d_s, d_r, x_s, x_r, y_s, y_r, known_sem,
):
    ng = nz * NY // GROUP
    nsp = nz * NY
    sp = lax.axis_index("sp")
    tp = lax.axis_index("tp")
    m, g = lax.rem(sp, GROUP), lax.div(sp, GROUP)
    y, zz = lax.rem(sp, NY), lax.div(sp, NY)
    xx, core = lax.div(tp, 2), lax.rem(tp, 2)

    def at(s, t):
        return (s, t)

    prev = at(lax.rem(sp + nsp - 1, nsp), tp)
    nxt = at(lax.rem(sp + 1, nsp), tp)
    zprev = at(lax.rem(sp + nsp - NY, nsp), tp)
    znext = at(lax.rem(sp + NY, nsp), tp)
    partner = at(sp, tp + 1 - 2 * core)
    group_peer = [at(g * GROUP + lax.rem(m + d, GROUP), tp) for d in range(GROUP)]
    far_peer = [at(lax.rem(g + d, ng) * GROUP + m, tp) for d in range(ng)]
    y_peer = [at(zz * NY + lax.rem(y + d, NY), tp) for d in range(NY)]
    x_peer = [at(sp, lax.rem(xx + d, nx) * 2 + core) for d in range(nx)]

    barrier = pltpu.get_barrier_semaphore()
    known = [[at(lax.rem(sp + nsp + way * NY * hop, nsp), tp) for way in (1, -1)] for hop in (2, 4)]
    greeted = [prev, nxt, zprev, znext, partner] + group_peer[1:] + x_peer[1:] + known[0]
    for device in greeted:
        pl.semaphore_signal(barrier, inc=1, device_id=device, device_id_type=pl.DeviceIdType.MESH)

    sends = []

    def send(src, dst, ssem, rsem, device):
        copy = pltpu.make_async_remote_copy(
            src_ref=src, dst_ref=dst, send_sem=ssem, recv_sem=rsem,
            device_id=device, device_id_type=pl.DeviceIdType.MESH,
        )
        copy.start()
        sends.append(copy)

    def arrived(dst, ssem, rsem, device):
        pltpu.make_async_remote_copy(
            src_ref=dst, dst_ref=dst, send_sem=ssem, recv_sem=rsem,
            device_id=device, device_id_type=pl.DeviceIdType.MESH,
        ).wait_recv()

    lane = lax.broadcasted_iota(jnp.int32, (TOK, 128), 1)
    sub = lax.broadcasted_iota(jnp.int32, (TOK, 128), 0)
    low = lane < 64
    low1 = low[:1]

    wbuf[zz] = w_ref[...]

    row8 = lax.broadcasted_iota(jnp.int32, (8, 128), 0)
    raw = jnp.concatenate([raw_ref[0], raw_ref[1]], axis=0)
    spike = jnp.concatenate([spike_ref[0], spike_ref[1]], axis=0)
    speed = jnp.zeros((8, 128), F32)
    for i in range(8):
        speed = jnp.where(row8 == i, speed_ref[i // 4, i % 4], speed)
    step = jnp.maximum(raw, 0.0) + jnp.log(1.0 + jnp.exp(-jnp.abs(raw)))
    logdecay = -jnp.exp(speed) * step + spike
    upto = (sub <= lane).astype(F32)
    onward = (sub >= lane).astype(F32)
    cum_f = jnp.dot(logdecay, upto, precision=HIGHEST, preferred_element_type=F32)
    cum_b = jnp.dot(logdecay, onward, precision=HIGHEST, preferred_element_type=F32)
    cum = jnp.where(row8 < 4, cum_f, cum_b)
    total = jnp.broadcast_to(jnp.sum(logdecay, axis=1, keepdims=True), (8, 128))
    to_end = step * jnp.exp(total - cum)
    grown = jnp.exp(cum)
    whole = jnp.exp(total)
    columns = jnp.concatenate([cum, to_end, grown, jnp.zeros((104, 128), F32)], axis=0).T

    def spread(first):
        tiles = [
            jnp.where(low, columns[:, first + 2 * i : first + 2 * i + 1], columns[:, first + 2 * i + 1 : first + 2 * i + 2])
            for i in range(2)
        ]
        return jnp.concatenate(tiles, axis=1)

    def spread_row(first):
        tiles = [
            jnp.where(low1, whole[first + 2 * i : first + 2 * i + 1], whole[first + 2 * i + 1 : first + 2 * i + 2])
            for i in range(2)
        ]
        return jnp.concatenate(tiles, axis=1)

    row16 = lax.broadcasted_iota(jnp.int32, (16, 256), 0)

    def split_rows(values):
        rows = jnp.zeros((16, 256), F32)
        at_row = 0
        for value in values:
            rest = value
            for _ in range(3):
                piece = rest.astype(BF16).astype(F32)
                rows = jnp.where(row16 == at_row, piece, rows)
                rest = rest - piece
                at_row += 1
        return rows.astype(BF16)

    decay_rows = split_rows([spread_row(0), spread_row(4)])

    inner_cos, inner_sin = inner_ref[0], inner_ref[1]

    def turn(value, block):
        cosine = start_ref[sp + block, 0:1, :]
        sine = start_ref[sp + block, 1:2, :]
        here_cos = cosine * inner_cos - sine * inner_sin
        here_sin = sine * inner_cos + cosine * inner_sin
        here_sin = jnp.where(low, -here_sin, here_sin)
        value = value.astype(F32)
        return (value * here_cos + pltpu.roll(value, 64, 1) * here_sin).astype(BF16)

    queries = jnp.concatenate([turn(q_ref[:, 0:128], 1), turn(q_ref[:, 128:256], 1)], axis=0)
    pad[8 : 8 + TOK, 0:256] = x_ref[...].astype(F32)
    pad[8 : 8 + TOK, 256:384] = b_ref[...].astype(F32)
    pad[8 : 8 + TOK, 384:512] = c_ref[...].astype(F32)
    r2[g] = jnp.zeros((32, 256), BF16)

    pl.semaphore_wait(barrier, len(greeted))

    for i, (ref, buf) in enumerate([(x_ref, hx), (b_ref, hb), (c_ref, hc)]):
        send(ref.at[TOK - 16 : TOK], buf.at[0], halo_s.at[2 * i], halo_r.at[2 * i], nxt)
        send(ref.at[0:16], buf.at[1], halo_s.at[2 * i + 1], halo_r.at[2 * i + 1], prev)
    right_steps, left_steps = nz // 2, nz - 1 - nz // 2
    for half in range(2):
        send(w_ref.at[half], wbuf.at[zz, half], w_s.at[0, half, 0], w_r.at[0, half, 1], znext)
        send(w_ref.at[half], wbuf.at[zz, half], w_s.at[1, half, 0], w_r.at[1, half, 1], zprev)
    for i, (ref, buf) in enumerate([(k_ref, kbuf), (v_ref, vbuf)]):
        send(ref, buf.at[0], halo_s.at[6 + 2 * i], halo_r.at[6 + 2 * i], nxt)
        send(ref, buf.at[1], halo_s.at[7 + 2 * i], halo_r.at[7 + 2 * i], prev)

    def meet(rank):
        for device in known[rank]:
            pl.semaphore_signal(known_sem.at[rank], inc=1, device_id=device, device_id_type=pl.DeviceIdType.MESH)

    meet(0)

    def relay(s):
        for half in range(2):
            for way, steps, source, target in ((0, right_steps, zprev, znext), (1, left_steps, znext, zprev)):
                if s <= steps:
                    piece = lax.rem(zz + nz - s, nz) if way == 0 else lax.rem(zz + s, nz)
                    block = wbuf.at[piece, half]
                    arrived(block, w_s.at[way, half, 0], w_r.at[way, half, s], source)
                    if s < steps:
                        send(block, block, w_s.at[way, half, s], w_r.at[way, half, s + 1], target)

    has_prev, has_next = sp > 0, sp < nsp - 1
    for i, (buf, first, last) in enumerate([(hx, 0, 256), (hb, 256, 384), (hc, 384, 512)]):
        arrived(buf.at[0], halo_s.at[2 * i], halo_r.at[2 * i], prev)
        arrived(buf.at[1], halo_s.at[2 * i + 1], halo_r.at[2 * i + 1], nxt)
        before = buf[0].astype(F32)[8:16]
        after = buf[1].astype(F32)[0:8]
        pad[0:8, first:last] = jnp.where(has_prev, before, 0.0)
        pad[8 + TOK : 16 + TOK, first:last] = jnp.where(has_next, after, 0.0)

    def convolved(first, last, taps_ref):
        taps = taps_ref[...].astype(F32)
        summed = jnp.zeros((TOK, last - first), F32)
        for k in range(CONV):
            summed = summed + pad[6 + k : 6 + k + TOK, first:last] * taps[k : k + 1]
        return (summed / (1.0 + jnp.exp(-summed))).astype(BF16)

    xs = convolved(0, 256, tx_ref)
    writes = convolved(256, 384, tb_ref)
    reads = convolved(384, 512, tc_ref)

    pl.semaphore_wait(known_sem.at[0], 2)
    meet(1)

    xs32 = xs.astype(F32)
    ends = jnp.concatenate([xs32 * spread(8), xs32 * spread(12)], axis=1).astype(BF16)
    states = lax.dot_general(
        writes, ends, (((0,), (0,)), ((), ())), preferred_element_type=F32
    ).astype(BF16)
    for j in range(GROUP):
        s1[j, 0:16] = states[16 * j : 16 * j + 16, 0:256]
        s1[j, 16:32] = states[16 * j : 16 * j + 16, 256:512]
        s1[j, 32:48] = decay_rows
    for d in range(1, GROUP):
        send(s1.at[lax.rem(m + d, GROUP)], r1.at[m], s1s.at[d], s1r.at[d], group_peer[d])
    r1[m] = s1[m]

    relay(1)

    for i, buf in enumerate([kbuf, vbuf]):
        arrived(buf.at[0], halo_s.at[6 + 2 * i], halo_r.at[6 + 2 * i], prev)
        arrived(buf.at[1], halo_s.at[7 + 2 * i], halo_r.at[7 + 2 * i], nxt)
    keys = jnp.concatenate([turn(kbuf[0], 0), turn(k_ref[...], 1), turn(kbuf[1], 2)], axis=0)
    values = jnp.concatenate([vbuf[0], v_ref[...], vbuf[1]], axis=0)
    scores = nt(queries, keys) * HEAD ** (-0.5)
    i_q = lax.broadcasted_iota(jnp.int32, (2 * TOK, 3 * TOK), 0) & (TOK - 1)
    j_k = lax.broadcasted_iota(jnp.int32, (2 * TOK, 3 * TOK), 1)
    first_key = jnp.where(has_prev, 0, TOK)
    last_key = jnp.where(has_next, 3 * TOK, 2 * TOK)
    allowed = (jnp.abs(j_k - TOK - i_q) <= WINDOW) & (j_k >= first_key) & (j_k < last_key)
    scores = jnp.where(allowed, scores, -1e30)
    head_row = lax.broadcasted_iota(jnp.int32, (2 * TOK, 1), 0)
    sink = jnp.where(head_row < TOK, sink_ref[0], sink_ref[1])
    top = jnp.maximum(jnp.max(scores, axis=1, keepdims=True), sink)
    weights = jnp.exp(scores - top)
    denominator = jnp.sum(weights, axis=1, keepdims=True) + jnp.exp(sink - top)
    probabilities = (weights / denominator).astype(BF16)
    attended = jnp.dot(probabilities, values, preferred_element_type=F32).astype(BF16)
    act[0, 0, :, 0:128] = attended[0:TOK]
    act[0, 0, :, 128:256] = attended[TOK : 2 * TOK]
    for d in (1, 3, 2):
        send(act.at[0, 0], act.at[NY - d, 0], a_s.at[0, d], a_r.at[0, NY - d], y_peer[d])

    relay(2)
    relay(3)

    for d in range(1, GROUP):
        arrived(r1.at[lax.rem(m + GROUP - d, GROUP)], s1s.at[d], s1r.at[d], group_peer[d])
    fades = [r1[j, 32:48].astype(F32) for j in range(GROUP)]
    fade_f = [f[0:1] + f[1:2] + f[2:3] for f in fades]
    fade_b = [f[3:4] + f[4:5] + f[5:6] for f in fades]
    run, fade = jnp.zeros((16, 256), F32), jnp.ones((1, 256), F32)
    for j in range(GROUP):
        pf[j] = run
        cf[j] = jnp.broadcast_to(fade, (8, 256))
        run = run * fade_f[j] + r1[j, 0:16].astype(F32)
        fade = fade * fade_f[j]
    s2[0, 0:16] = run.astype(BF16)
    s2[0, 16:32] = split_rows([fade])
    run, fade = jnp.zeros((16, 256), F32), jnp.ones((1, 256), F32)
    for j in reversed(range(GROUP)):
        pb[j] = run
        cb[j] = jnp.broadcast_to(fade, (8, 256))
        run = run * fade_b[j] + r1[j, 16:32].astype(F32)
        fade = fade * fade_b[j]
    s2[1, 0:16] = run.astype(BF16)
    s2[1, 16:32] = split_rows([fade])
    pl.semaphore_wait(known_sem.at[1], 2)
    for d in range(1, ng):
        other = lax.rem(g + d, ng)
        way = jnp.where(other > g, 0, 1)
        send(s2.at[way], r2.at[g], s2s.at[d], s2r.at[d], far_peer[d])

    affinity = nt(reads, writes)
    for h in range(4):
        ahead = columns[:, h : h + 1] - cum[h : h + 1]
        back = columns[:, 4 + h : 5 + h] - cum[4 + h : 5 + h]
        fading = jnp.exp(jnp.where(lane <= sub, ahead, back))
        step_f, step_b = step[h : h + 1], step[4 + h : 5 + h]
        size = jnp.where(lane < sub, step_f, jnp.where(lane > sub, step_b, step_f + step_b))
        mix = (affinity * fading * size).astype(BF16)
        yw[:, 64 * h : 64 * h + 64] = jnp.dot(mix, xs[:, 64 * h : 64 * h + 64], preferred_element_type=F32)

    relay(4)
    relay(5)
    relay(6)

    for d in range(1, ng):
        arrived(r2.at[lax.rem(g + ng - d, ng)], s2s.at[d], s2r.at[d], far_peer[d])
    come_f, come_b = jnp.zeros((16, 256), F32), jnp.zeros((16, 256), F32)
    for j in range(ng):
        f = r2[j, 16:32].astype(F32)
        come_f = jnp.where(j < g, come_f * (f[0:1] + f[1:2] + f[2:3]) + r2[j, 0:16].astype(F32), come_f)
    for j in reversed(range(ng)):
        f = r2[j, 16:32].astype(F32)
        come_b = jnp.where(j > g, come_b * (f[0:1] + f[1:2] + f[2:3]) + r2[j, 0:16].astype(F32), come_b)
    for j in range(GROUP):
        s3[j, 0:16] = (come_f * cf[j, 0:1] + pf[j]).astype(BF16)
        s3[j, 16:32] = (come_b * cb[j, 0:1] + pb[j]).astype(BF16)
    for d in range(1, GROUP):
        send(s3.at[lax.rem(m + d, GROUP)], r3.at[m], s3s.at[d], s3r.at[d], group_peer[d])
    r3[m] = s3[m]

    for s in range(7, right_steps + 1):
        relay(s)

    for d in range(1, GROUP):
        arrived(r3.at[lax.rem(m + GROUP - d, GROUP)], s3s.at[d], s3r.at[d], group_peer[d])
    in_f = r3[:, 0:16].reshape(128, 256)
    in_b = r3[:, 16:32].reshape(128, 256)
    both = (
        yw[...]
        + jnp.dot(reads, in_f, preferred_element_type=F32) * spread(16)
        + jnp.dot(reads, in_b, preferred_element_type=F32) * spread(20)
    )
    gate = z_ref[...].astype(F32)
    gated = both * (gate / (1.0 + jnp.exp(-gate)))
    mean = jnp.sum(gated * gated, axis=1, keepdims=True) * (1.0 / 256)
    act[0, 1] = (gated * lax.rsqrt(mean + EPSILON) * gain_ref[...]).astype(BF16)
    for d in (1, 3, 2):
        send(act.at[0, 1], act.at[NY - d, 1], a_s.at[1, d], a_r.at[1, NY - d], y_peer[d])


    def pair_sum(e):
        arrived(prx.at[e], d_s.at[e], d_r.at[e], partner)
        for c in range(nx):
            rows = slice(16 * c, 16 * c + 16)
            xbuf[e, c] = (pbuf[e, core, rows].astype(F32) + prx[e, rows].astype(F32)).astype(BF16)
        for d in range(1, nx):
            send(xbuf.at[e, lax.rem(xx + d, nx)], xrx.at[e, d], x_s.at[e, d], x_r.at[e, d], x_peer[d])

    order = (0, 1, 3, 2)
    for i, e in enumerate(order):
        if e:
            arrived(act.at[e, 0], a_s.at[0, e], a_r.at[0, e], y_peer[e])
            arrived(act.at[e, 1], a_s.at[1, e], a_r.at[1, e], y_peer[e])
        for n in range(nz // 4):
            part = nt(act[e, 0], wbuf[4 * n : 4 * n + 4, 0].reshape(256, 256))
            part = part + nt(act[e, 1], wbuf[4 * n : 4 * n + 4, 1].reshape(256, 256))
            part = part.astype(BF16)
            for c in range(nx):
                for k in range(2):
                    pbuf[e, k, 16 * c : 16 * c + 16, 256 * n : 256 * n + 256] = part[
                        32 * c + 16 * k : 32 * c + 16 * k + 16
                    ]
        send(pbuf.at[e, 1 - core], prx.at[e], d_s.at[e], d_r.at[e], partner)
        if i:
            pair_sum(order[i - 1])
    pair_sum(order[-1])

    for e in order:
        done = xbuf[e, xx].astype(F32)
        for d in range(1, nx):
            arrived(xrx.at[e, d], x_s.at[e, d], x_r.at[e, d], x_peer[d])
            done = done + xrx[e, d].astype(F32)
        if e:
            fin[e] = done.astype(BF16)
            send(fin.at[e], ybuf.at[y], y_s.at[e], y_r.at[NY - e], y_peer[e])
        else:
            ybuf[y] = done.astype(BF16)
    for e in (1, 3, 2):
        arrived(ybuf.at[lax.rem(y + e, NY)], y_s.at[e], y_r.at[e], y_peer[e])
    for p in range(nz // 2):
        cells = [ybuf[j, :, 128 * p : 128 * p + 128] for j in range(NY)]
        for half in range(2):
            for pair in range(2):
                first = 256 * (2 * p + half) + 128 * pair
                o_ref[:, first : first + 128] = jnp.concatenate(
                    [cells[2 * pair + i][:, 64 * half : 64 * half + 64] for i in range(2)], axis=1
                )
    for copy in sends:
        copy.wait_send()


def solution(mesh):
    nz = mesh.shape["sp"] // NY
    nx = mesh.shape["tp"] // 2
    starts, inner = rotary_tables(mesh.shape["sp"])

    def local(
        asking, matching, carried, switch, source, storing, fetching,
        duality_taps, storing_taps, fetching_taps, raw, speeds, spikes, sinks, gains, mapping,
    ):
        cols = 64 * nz
        vmem = pl.BlockSpec(memory_space=pltpu.VMEM)
        smem = pl.BlockSpec(memory_space=pltpu.SMEM)
        dma = pltpu.SemaphoreType.DMA
        ng = nz * NY // GROUP
        rings = nz // 2 + 1
        scratch = [
            pltpu.VMEM((2, TOK, 128), BF16), pltpu.VMEM((2, TOK, 128), BF16),
            pltpu.VMEM((2, 16, 256), BF16), pltpu.VMEM((2, 16, 128), BF16), pltpu.VMEM((2, 16, 128), BF16),
            pltpu.VMEM((TOK + 16, 512), F32), pltpu.VMEM((TOK, 256), F32),
            pltpu.VMEM((GROUP, 48, 256), BF16), pltpu.VMEM((GROUP, 48, 256), BF16),
            pltpu.VMEM((2, 32, 256), BF16), pltpu.VMEM((ng, 32, 256), BF16),
            pltpu.VMEM((GROUP, 32, 256), BF16), pltpu.VMEM((GROUP, 32, 256), BF16),
            pltpu.VMEM((GROUP, 16, 256), F32), pltpu.VMEM((GROUP, 8, 256), F32),
            pltpu.VMEM((GROUP, 16, 256), F32), pltpu.VMEM((GROUP, 8, 256), F32),
            pltpu.VMEM((nz, 2, 64, 256), BF16),
            pltpu.VMEM((NY, 2, TOK, 256), BF16),
            pltpu.VMEM((NY, 2, 16 * nx, cols), BF16), pltpu.VMEM((NY, 16 * nx, cols), BF16),
            pltpu.VMEM((NY, nx, 16, cols), BF16), pltpu.VMEM((NY, nx, 16, cols), BF16),
            pltpu.VMEM((NY, 16, cols), BF16), pltpu.VMEM((NY, 16, cols), BF16),
            dma((10,)), dma((10,)), dma((2, 2, rings)), dma((2, 2, rings)),
            dma((GROUP,)), dma((GROUP,)), dma((ng,)), dma((ng,)), dma((GROUP,)), dma((GROUP,)),
            dma((2, NY)), dma((2, NY)), dma((NY,)), dma((NY,)),
            dma((NY, nx)), dma((NY, nx)), dma((NY,)), dma((NY,)), pltpu.SemaphoreType.REGULAR((2,)),
        ]
        return pl.pallas_call(
            functools.partial(kernel, nz, nx),
            out_shape=jax.ShapeDtypeStruct((TOK // (2 * nx), 4 * cols), BF16),
            in_specs=[vmem] * 12 + [smem, smem] + [vmem] * 4,
            out_specs=vmem,
            scratch_shapes=scratch,
            compiler_params=pltpu.CompilerParams(collective_id=0, has_side_effects=True),
        )(
            asking, matching, carried, switch, source, storing, fetching,
            duality_taps, storing_taps, fetching_taps, raw, spikes, speeds, sinks,
            gains.reshape(1, 256), jnp.swapaxes(mapping, 1, 2), jnp.asarray(starts), jnp.asarray(inner),
        )

    return jax.shard_map(
        local,
        mesh=mesh,
        in_specs=(
            P("sp", "tp"), P("sp", "tp"), P("sp", "tp"), P("sp", "tp"), P("sp", "tp"), P("sp", "tp"), P("sp", "tp"),
            P(None, "tp"), P(None, "tp"), P(None, "tp"),
            P(None, "tp", "sp"), P(None, "tp"), P(None, "tp", "sp"), P("tp"), P("tp"), P(None, "tp", "sp"),
        ),
        out_specs=P(("sp", "tp"), None),
        check_vma=False,
    )
```

```python
import functools

import jax
import jax.numpy as jnp
import numpy as np
from jax import lax
from jax.experimental import pallas as pl
from jax.experimental.pallas import tpu as pltpu
from jax.sharding import PartitionSpec as P

HEAD = 128
TOK = 128
CONV = 5
WINDOW = 128
NY = 4
GROUP = 8
F32 = jnp.float32
BF16 = jnp.bfloat16
ROTARY_BASE = 500000.0
EPSILON = 1e-06
HIGHEST = lax.Precision.HIGHEST


def rotary_tables(blocks):
    half = HEAD // 2
    spacing = ROTARY_BASE ** (-np.arange(half, dtype=np.float64) * 2.0 / HEAD)
    spacing = np.concatenate([spacing, spacing])
    starts = (np.arange(blocks + 2, dtype=np.float64) - 1.0)[:, None] * TOK * spacing[None, :]
    inner = np.arange(TOK, dtype=np.float64)[:, None] * spacing[None, :]
    starts = np.stack([np.cos(starts), np.sin(starts)], axis=1).astype(np.float32)
    inner = np.stack([np.cos(inner), np.sin(inner)]).astype(np.float32)
    return starts, inner


def nt(a, b, **kw):
    return lax.dot_general(a, b, (((1,), (1,)), ((), ())), preferred_element_type=F32, **kw)


def kernel(
    nz, nx,
    q_hbm, k_hbm, v_hbm, z_hbm, x_hbm, b_hbm, c_hbm, tx_hbm, tb_hbm, tc_hbm,
    raw_hbm, spike_hbm, speed_hbm, sink_hbm, gain_hbm, w_hbm, start_hbm, inner_hbm,
    o_ref,
    q_ref, k_ref, v_ref, z_ref, x_ref, b_ref, c_ref, tx_ref, tb_ref, tc_ref,
    raw_ref, spike_ref, speed_ref, sink_ref, gain_ref, w_ref, start_ref, inner_ref, in_sem,
    kbuf, vbuf, hx, hb, hc, pad, yw,
    s1, r1, s2, r2, s3, r3, pf, cf, pb, cb,
    wbuf, act, pbuf, prx, xbuf, xrx, via, both_x, fin, ybuf,
    halo_s, halo_r, w_s, w_r, s1s, s1r, s2s, s2r, s3s, s3r,
    a_s, a_r, d_s, d_r, x_s, x_r, y_s, y_r, known_sem,
):
    ng = nz * NY // GROUP
    nsp = nz * NY
    sp = lax.axis_index("sp")
    tp = lax.axis_index("tp")
    m, g = lax.rem(sp, GROUP), lax.div(sp, GROUP)
    y, zz = lax.rem(sp, NY), lax.div(sp, NY)
    xx, core = lax.div(tp, 2), lax.rem(tp, 2)

    def at(s, t):
        return (s, t)

    prev = at(lax.rem(sp + nsp - 1, nsp), tp)
    nxt = at(lax.rem(sp + 1, nsp), tp)
    zprev = at(lax.rem(sp + nsp - NY, nsp), tp)
    znext = at(lax.rem(sp + NY, nsp), tp)
    partner = at(sp, tp + 1 - 2 * core)
    group_peer = [at(g * GROUP + lax.rem(m + d, GROUP), tp) for d in range(GROUP)]
    far_peer = [at(lax.rem(g + d, ng) * GROUP + m, tp) for d in range(ng)]
    y_peer = [at(zz * NY + lax.rem(y + d, NY), tp) for d in range(NY)]
    x_peer = [at(sp, lax.rem(xx + d, nx) * 2 + core) for d in range(nx)]

    barrier = pltpu.get_barrier_semaphore()
    known = [[at(lax.rem(sp + nsp + way * NY * hop, nsp), tp) for way in (1, -1)] for hop in (2, 4)]
    greeted = [prev, nxt, zprev, znext, partner] + group_peer[1:] + x_peer[1:] + known[0]
    for device in greeted:
        pl.semaphore_signal(barrier, inc=1, device_id=device, device_id_type=pl.DeviceIdType.MESH)

    pairs = [
        (x_hbm, x_ref), (b_hbm, b_ref), (c_hbm, c_ref), (w_hbm, w_ref), (k_hbm, k_ref), (v_hbm, v_ref),
        (raw_hbm, raw_ref), (spike_hbm, spike_ref), (speed_hbm, speed_ref), (q_hbm, q_ref), (inner_hbm, inner_ref),
        (start_hbm.at[pl.ds(sp, 3)], start_ref), (tx_hbm, tx_ref), (tb_hbm, tb_ref), (tc_hbm, tc_ref),
        (sink_hbm, sink_ref), (z_hbm, z_ref), (gain_hbm, gain_ref),
    ]
    inputs = [pltpu.make_async_copy(src, dst, in_sem.at[i]) for i, (src, dst) in enumerate(pairs)]
    for copy in inputs:
        copy.start()

    sends = []

    def send(src, dst, ssem, rsem, device):
        copy = pltpu.make_async_remote_copy(
            src_ref=src, dst_ref=dst, send_sem=ssem, recv_sem=rsem,
            device_id=device, device_id_type=pl.DeviceIdType.MESH,
        )
        copy.start()
        sends.append(copy)

    def arrived(dst, ssem, rsem, device):
        pltpu.make_async_remote_copy(
            src_ref=dst, dst_ref=dst, send_sem=ssem, recv_sem=rsem,
            device_id=device, device_id_type=pl.DeviceIdType.MESH,
        ).wait_recv()

    lane = lax.broadcasted_iota(jnp.int32, (TOK, 128), 1)
    sub = lax.broadcasted_iota(jnp.int32, (TOK, 128), 0)
    low = lane < 64
    low1 = low[:1]

    for copy in inputs[:6]:
        copy.wait()
    pl.semaphore_wait(barrier, len(greeted))

    for i, (ref, buf) in enumerate([(x_ref, hx), (b_ref, hb), (c_ref, hc)]):
        send(ref.at[TOK - 16 : TOK], buf.at[0], halo_s.at[2 * i], halo_r.at[2 * i], nxt)
        send(ref.at[0:16], buf.at[1], halo_s.at[2 * i + 1], halo_r.at[2 * i + 1], prev)
    right_steps, left_steps = nz // 2, nz - 1 - nz // 2
    for half in range(2):
        send(w_ref.at[half], wbuf.at[zz, half], w_s.at[0, half, 0], w_r.at[0, half, 1], znext)
        send(w_ref.at[half], wbuf.at[zz, half], w_s.at[1, half, 0], w_r.at[1, half, 1], zprev)
    for i, (ref, buf) in enumerate([(k_ref, kbuf), (v_ref, vbuf)]):
        send(ref, buf.at[0], halo_s.at[6 + 2 * i], halo_r.at[6 + 2 * i], nxt)
        send(ref, buf.at[1], halo_s.at[7 + 2 * i], halo_r.at[7 + 2 * i], prev)

    def meet(rank):
        for device in known[rank]:
            pl.semaphore_signal(known_sem.at[rank], inc=1, device_id=device, device_id_type=pl.DeviceIdType.MESH)

    meet(0)

    def relay(s):
        for half in range(2):
            for way, steps, source, target in ((0, right_steps, zprev, znext), (1, left_steps, znext, zprev)):
                if s <= steps:
                    piece = lax.rem(zz + nz - s, nz) if way == 0 else lax.rem(zz + s, nz)
                    block = wbuf.at[piece, half]
                    arrived(block, w_s.at[way, half, 0], w_r.at[way, half, s], source)
                    if s < steps:
                        send(block, block, w_s.at[way, half, s], w_r.at[way, half, s + 1], target)

    for copy in inputs[6:]:
        copy.wait()
    wbuf[zz] = w_ref[...]

    row8 = lax.broadcasted_iota(jnp.int32, (8, 128), 0)
    raw = jnp.concatenate([raw_ref[0], raw_ref[1]], axis=0)
    spike = jnp.concatenate([spike_ref[0], spike_ref[1]], axis=0)
    speed = jnp.zeros((8, 128), F32)
    for i in range(8):
        speed = jnp.where(row8 == i, speed_ref[i // 4 : i // 4 + 1, i % 4 : i % 4 + 1], speed)
    step = jnp.maximum(raw, 0.0) + jnp.log(1.0 + jnp.exp(-jnp.abs(raw)))
    logdecay = -jnp.exp(speed) * step + spike
    upto = (sub <= lane).astype(F32)
    onward = (sub >= lane).astype(F32)
    cum_f = jnp.dot(logdecay, upto, precision=HIGHEST, preferred_element_type=F32)
    cum_b = jnp.dot(logdecay, onward, precision=HIGHEST, preferred_element_type=F32)
    cum = jnp.where(row8 < 4, cum_f, cum_b)
    total = jnp.broadcast_to(jnp.sum(logdecay, axis=1, keepdims=True), (8, 128))
    to_end = step * jnp.exp(total - cum)
    grown = jnp.exp(cum)
    whole = jnp.exp(total)
    columns = jnp.concatenate([cum, to_end, grown, jnp.zeros((104, 128), F32)], axis=0).T

    def spread(first):
        tiles = [
            jnp.where(low, columns[:, first + 2 * i : first + 2 * i + 1], columns[:, first + 2 * i + 1 : first + 2 * i + 2])
            for i in range(2)
        ]
        return jnp.concatenate(tiles, axis=1)

    def spread_row(first):
        tiles = [
            jnp.where(low1, whole[first + 2 * i : first + 2 * i + 1], whole[first + 2 * i + 1 : first + 2 * i + 2])
            for i in range(2)
        ]
        return jnp.concatenate(tiles, axis=1)

    row16 = lax.broadcasted_iota(jnp.int32, (16, 128), 0)

    def split_rows(values):
        rows = jnp.zeros((16, 128), F32)
        at_row = 0
        for value in values:
            for first in (0, 128):
                rest = value[:, first : first + 128]
                for _ in range(3):
                    piece = rest.astype(BF16).astype(F32)
                    rows = jnp.where(row16 == at_row, piece, rows)
                    rest = rest - piece
                    at_row += 1
        return rows.astype(BF16)

    def joined_rows(rows, first):
        rows = rows.astype(F32)
        tiles = [rows[i : i + 1] + rows[i + 1 : i + 2] + rows[i + 2 : i + 3] for i in (first, first + 3)]
        return jnp.concatenate(tiles, axis=1)

    def wide(ref, j, first):
        tiles = [ref[j, first + 16 * i : first + 16 * i + 16].astype(F32) for i in range(2)]
        return jnp.concatenate(tiles, axis=1)

    def narrow(ref, j, first, value):
        for i in range(2):
            ref[j, first + 16 * i : first + 16 * i + 16] = value[:, 128 * i : 128 * i + 128].astype(BF16)

    decay_rows = split_rows([spread_row(0), spread_row(4)])

    inner_cos, inner_sin = inner_ref[0], inner_ref[1]

    def turn(value, block):
        cosine = start_ref[block, 0:1, :]
        sine = start_ref[block, 1:2, :]
        here_cos = cosine * inner_cos - sine * inner_sin
        here_sin = sine * inner_cos + cosine * inner_sin
        here_sin = jnp.where(low, -here_sin, here_sin)
        value = value.astype(F32)
        return (value * here_cos + pltpu.roll(value, 64, 1) * here_sin).astype(BF16)

    queries = jnp.concatenate([turn(q_ref[:, 0:128], 1), turn(q_ref[:, 128:256], 1)], axis=0)
    pad[8 : 8 + TOK, 0:256] = x_ref[...].astype(F32)
    pad[8 : 8 + TOK, 256:384] = b_ref[...].astype(F32)
    pad[8 : 8 + TOK, 384:512] = c_ref[...].astype(F32)
    r2[g] = jnp.zeros((48, 128), BF16)

    relay(1)

    has_prev, has_next = sp > 0, sp < nsp - 1
    for i, (buf, first, last) in enumerate([(hx, 0, 256), (hb, 256, 384), (hc, 384, 512)]):
        arrived(buf.at[0], halo_s.at[2 * i], halo_r.at[2 * i], prev)
        arrived(buf.at[1], halo_s.at[2 * i + 1], halo_r.at[2 * i + 1], nxt)
        before = buf[0].astype(F32)[8:16]
        after = buf[1].astype(F32)[0:8]
        pad[0:8, first:last] = jnp.where(has_prev, before, 0.0)
        pad[8 + TOK : 16 + TOK, first:last] = jnp.where(has_next, after, 0.0)

    def convolved(first, last, taps_ref):
        taps = taps_ref[...].astype(F32)
        summed = jnp.zeros((TOK, last - first), F32)
        for k in range(CONV):
            summed = summed + pad[6 + k : 6 + k + TOK, first:last] * taps[k : k + 1]
        return (summed / (1.0 + jnp.exp(-summed))).astype(BF16)

    xs = convolved(0, 256, tx_ref)
    writes = convolved(256, 384, tb_ref)
    reads = convolved(384, 512, tc_ref)

    xs32 = xs.astype(F32)
    ends = jnp.concatenate([xs32 * spread(8), xs32 * spread(12)], axis=1).astype(BF16)
    states = lax.dot_general(
        writes, ends, (((0,), (0,)), ((), ())), preferred_element_type=F32
    ).astype(BF16)
    for j in range(GROUP):
        for i in range(4):
            s1[j, 16 * i : 16 * i + 16] = states[16 * j : 16 * j + 16, 128 * i : 128 * i + 128]
        s1[j, 64:80] = decay_rows
    for d in range(1, GROUP):
        send(s1.at[lax.rem(m + d, GROUP)], r1.at[m], s1s.at[d], s1r.at[d], group_peer[d])
    r1[m] = s1[m]
    pl.semaphore_wait(known_sem.at[0], 2)
    meet(1)

    relay(2)

    for i, buf in enumerate([kbuf, vbuf]):
        arrived(buf.at[0], halo_s.at[6 + 2 * i], halo_r.at[6 + 2 * i], prev)
        arrived(buf.at[1], halo_s.at[7 + 2 * i], halo_r.at[7 + 2 * i], nxt)
    keys = jnp.concatenate([turn(kbuf[0], 0), turn(k_ref[...], 1), turn(kbuf[1], 2)], axis=0)
    values = jnp.concatenate([vbuf[0], v_ref[...], vbuf[1]], axis=0)
    scores = nt(queries, keys) * HEAD ** (-0.5)
    i_q = lax.broadcasted_iota(jnp.int32, (2 * TOK, 3 * TOK), 0) & (TOK - 1)
    j_k = lax.broadcasted_iota(jnp.int32, (2 * TOK, 3 * TOK), 1)
    first_key = jnp.where(has_prev, 0, TOK)
    last_key = jnp.where(has_next, 3 * TOK, 2 * TOK)
    allowed = (jnp.abs(j_k - TOK - i_q) <= WINDOW) & (j_k >= first_key) & (j_k < last_key)
    scores = jnp.where(allowed, scores, -1e30)
    head_row = lax.broadcasted_iota(jnp.int32, (2 * TOK, 1), 0)
    sink = jnp.where(head_row < TOK, sink_ref[0:1, 0:1], sink_ref[0:1, 1:2])
    top = jnp.maximum(jnp.max(scores, axis=1, keepdims=True), sink)
    weights = jnp.exp(scores - top)
    denominator = jnp.sum(weights, axis=1, keepdims=True) + jnp.exp(sink - top)
    probabilities = (weights / denominator).astype(BF16)
    attended = jnp.dot(probabilities, values, preferred_element_type=F32).astype(BF16)
    act[0, 0, :, 0:128] = attended[0:TOK]
    act[0, 0, :, 128:256] = attended[TOK : 2 * TOK]
    for d in (1, 3, 2):
        send(act.at[0, 0], act.at[NY - d, 0], a_s.at[0, d], a_r.at[0, NY - d], y_peer[d])

    relay(3)

    for d in range(1, GROUP):
        arrived(r1.at[lax.rem(m + GROUP - d, GROUP)], s1s.at[d], s1r.at[d], group_peer[d])
    fade_f = [joined_rows(r1[j, 64:80], 0) for j in range(GROUP)]
    fade_b = [joined_rows(r1[j, 64:80], 6) for j in range(GROUP)]
    run, fade = jnp.zeros((16, 256), F32), jnp.ones((1, 256), F32)
    for j in range(GROUP):
        pf[j] = run
        cf[j] = jnp.broadcast_to(fade, (8, 256))
        run = run * fade_f[j] + wide(r1, j, 0)
        fade = fade * fade_f[j]
    narrow(s2, 0, 0, run)
    s2[0, 32:48] = split_rows([fade])
    run, fade = jnp.zeros((16, 256), F32), jnp.ones((1, 256), F32)
    for j in reversed(range(GROUP)):
        pb[j] = run
        cb[j] = jnp.broadcast_to(fade, (8, 256))
        run = run * fade_b[j] + wide(r1, j, 32)
        fade = fade * fade_b[j]
    narrow(s2, 1, 0, run)
    s2[1, 32:48] = split_rows([fade])
    pl.semaphore_wait(known_sem.at[1], 2)
    for d in range(1, ng):
        other = lax.rem(g + d, ng)
        way = jnp.where(other > g, 0, 1)
        send(s2.at[way], r2.at[g], s2s.at[d], s2r.at[d], far_peer[d])

    affinity = nt(reads, writes)
    for h in range(4):
        ahead = columns[:, h : h + 1] - cum[h : h + 1]
        back = columns[:, 4 + h : 5 + h] - cum[4 + h : 5 + h]
        fading = jnp.exp(jnp.where(lane <= sub, ahead, back))
        step_f, step_b = step[h : h + 1], step[4 + h : 5 + h]
        size = jnp.where(lane < sub, step_f, jnp.where(lane > sub, step_b, step_f + step_b))
        mix = (affinity * fading * size).astype(BF16)
        yw[:, 64 * h : 64 * h + 64] = jnp.dot(mix, xs[:, 64 * h : 64 * h + 64], preferred_element_type=F32)

    relay(4)
    relay(5)
    relay(6)

    for d in range(1, ng):
        arrived(r2.at[lax.rem(g + ng - d, ng)], s2s.at[d], s2r.at[d], far_peer[d])
    come_f, come_b = jnp.zeros((16, 256), F32), jnp.zeros((16, 256), F32)
    for j in range(ng):
        come_f = jnp.where(j < g, come_f * joined_rows(r2[j, 32:48], 0) + wide(r2, j, 0), come_f)
    for j in reversed(range(ng)):
        come_b = jnp.where(j > g, come_b * joined_rows(r2[j, 32:48], 0) + wide(r2, j, 0), come_b)
    for j in range(GROUP):
        narrow(s3, j, 0, come_f * cf[j, 0:1] + pf[j])
        narrow(s3, j, 32, come_b * cb[j, 0:1] + pb[j])
    for d in range(1, GROUP):
        send(s3.at[lax.rem(m + d, GROUP)], r3.at[m], s3s.at[d], s3r.at[d], group_peer[d])
    r3[m] = s3[m]

    for s in range(7, right_steps + 1):
        relay(s)

    for d in range(1, GROUP):
        arrived(r3.at[lax.rem(m + GROUP - d, GROUP)], s3s.at[d], s3r.at[d], group_peer[d])
    tiles = [r3[:, 16 * i : 16 * i + 16].reshape(128, 128) for i in range(4)]
    in_f = jnp.concatenate(tiles[:2], axis=1)
    in_b = jnp.concatenate(tiles[2:], axis=1)
    both = (
        yw[...]
        + jnp.dot(reads, in_f, preferred_element_type=F32) * spread(16)
        + jnp.dot(reads, in_b, preferred_element_type=F32) * spread(20)
    )
    gate = z_ref[...].astype(F32)
    gated = both * (gate / (1.0 + jnp.exp(-gate)))
    mean = jnp.sum(gated * gated, axis=1, keepdims=True) * (1.0 / 256)
    act[0, 1] = (gated * lax.rsqrt(mean + EPSILON) * gain_ref[...]).astype(BF16)
    for d in (1, 3, 2):
        send(act.at[0, 1], act.at[NY - d, 1], a_s.at[1, d], a_r.at[1, NY - d], y_peer[d])


    order = (0, 1, 3, 2)
    via_step = {0: 3, 1: 1, 3: 3, 2: 0}

    def chunk(e, d):
        return xbuf.at[e, lax.rem(xx + d, nx)]

    def pair_sum(e):
        arrived(prx.at[e], d_s.at[e], d_r.at[e], partner)
        for c in range(nx):
            rows = slice(16 * c, 16 * c + 16)
            xbuf[e, c] = (pbuf[e, core, rows].astype(F32) + prx[e, rows].astype(F32)).astype(BF16)
        step_to = via_step[e]
        if step_to:
            send(chunk(e, 2), via.at[e], x_s.at[e, 2], x_r.at[e, 2], x_peer[step_to])
            send(chunk(e, 4 - step_to), xrx.at[e, 4 - step_to], x_s.at[e, 4 - step_to], x_r.at[e, 4 - step_to], x_peer[4 - step_to])
        else:
            for d in (2, 1, 3):
                send(chunk(e, d), xrx.at[e, d], x_s.at[e, d], x_r.at[e, d], x_peer[d])

    def pass_on(e):
        step_to = via_step[e]
        if step_to:
            arrived(via.at[e], x_s.at[e, 2], x_r.at[e, 2], x_peer[step_to])
            both_x[e] = (xbuf[e, lax.rem(xx + step_to, nx)].astype(F32) + via[e].astype(F32)).astype(BF16)
            send(both_x.at[e], xrx.at[e, step_to], x_s.at[e, step_to], x_r.at[e, step_to], x_peer[step_to])

    for i, e in enumerate(order):
        if e:
            arrived(act.at[e, 0], a_s.at[0, e], a_r.at[0, e], y_peer[e])
            arrived(act.at[e, 1], a_s.at[1, e], a_r.at[1, e], y_peer[e])
        for n in range(nz // 4):
            part = nt(act[e, 0], wbuf[4 * n : 4 * n + 4, 0].reshape(256, 256))
            part = part + nt(act[e, 1], wbuf[4 * n : 4 * n + 4, 1].reshape(256, 256))
            part = part.astype(BF16)
            for c in range(nx):
                for k in range(2):
                    pbuf[e, k, 16 * c : 16 * c + 16, 256 * n : 256 * n + 256] = part[
                        32 * c + 16 * k : 32 * c + 16 * k + 16
                    ]
        send(pbuf.at[e, 1 - core], prx.at[e], d_s.at[e], d_r.at[e], partner)
        if i >= 1:
            pair_sum(order[i - 1])
        if i >= 2:
            pass_on(order[i - 2])
    pair_sum(order[3])
    pass_on(order[2])

    for e in order:
        done = xbuf[e, xx].astype(F32)
        for d in (1, 3) if via_step[e] else (1, 3, 2):
            arrived(xrx.at[e, d], x_s.at[e, d], x_r.at[e, d], x_peer[d])
            done = done + xrx[e, d].astype(F32)
        if e:
            fin[e] = done.astype(BF16)
            send(fin.at[e], ybuf.at[y], y_s.at[e], y_r.at[NY - e], y_peer[e])
        else:
            ybuf[y] = done.astype(BF16)
    for e in (1, 3, 2):
        arrived(ybuf.at[lax.rem(y + e, NY)], y_s.at[e], y_r.at[e], y_peer[e])
    for p in range(nz // 2):
        cells = [ybuf[j, :, 128 * p : 128 * p + 128] for j in range(NY)]
        for half in range(2):
            for pair in range(2):
                first = 256 * (2 * p + half) + 128 * pair
                o_ref[:, first : first + 128] = jnp.concatenate(
                    [cells[2 * pair + i][:, 64 * half : 64 * half + 64] for i in range(2)], axis=1
                )
    for copy in sends:
        copy.wait_send()


def solution(mesh):
    nz = mesh.shape["sp"] // NY
    nx = mesh.shape["tp"] // 2
    starts, inner = rotary_tables(mesh.shape["sp"])

    def local(
        asking, matching, carried, switch, source, storing, fetching,
        duality_taps, storing_taps, fetching_taps, raw, speeds, spikes, sinks, gains, mapping,
    ):
        cols = 64 * nz
        vmem = pl.BlockSpec(memory_space=pltpu.VMEM)
        hbm = pl.BlockSpec(memory_space=pltpu.HBM)
        dma = pltpu.SemaphoreType.DMA
        ng = nz * NY // GROUP
        rings = nz // 2 + 1
        scratch = [
            pltpu.VMEM((TOK, 256), BF16), pltpu.VMEM((TOK, 128), BF16), pltpu.VMEM((TOK, 128), BF16),
            pltpu.VMEM((TOK, 256), BF16), pltpu.VMEM((TOK, 256), BF16), pltpu.VMEM((TOK, 128), BF16),
            pltpu.VMEM((TOK, 128), BF16), pltpu.VMEM((CONV, 256), BF16), pltpu.VMEM((CONV, 128), BF16),
            pltpu.VMEM((CONV, 128), BF16), pltpu.VMEM((2, 4, 128), F32), pltpu.VMEM((2, 4, 128), F32),
            pltpu.VMEM((2, 4), F32), pltpu.VMEM((1, 2), F32), pltpu.VMEM((1, 256), F32),
            pltpu.VMEM((2, 64, 256), BF16), pltpu.VMEM((3, 2, 128), F32), pltpu.VMEM((2, TOK, 128), F32), dma((18,)),
            pltpu.VMEM((2, TOK, 128), BF16), pltpu.VMEM((2, TOK, 128), BF16),
            pltpu.VMEM((2, 16, 256), BF16), pltpu.VMEM((2, 16, 128), BF16), pltpu.VMEM((2, 16, 128), BF16),
            pltpu.VMEM((TOK + 16, 512), F32), pltpu.VMEM((TOK, 256), F32),
            pltpu.VMEM((GROUP, 80, 128), BF16), pltpu.VMEM((GROUP, 80, 128), BF16),
            pltpu.VMEM((2, 48, 128), BF16), pltpu.VMEM((ng, 48, 128), BF16),
            pltpu.VMEM((GROUP, 64, 128), BF16), pltpu.VMEM((GROUP, 64, 128), BF16),
            pltpu.VMEM((GROUP, 16, 256), F32), pltpu.VMEM((GROUP, 8, 256), F32),
            pltpu.VMEM((GROUP, 16, 256), F32), pltpu.VMEM((GROUP, 8, 256), F32),
            pltpu.VMEM((nz, 2, 64, 256), BF16),
            pltpu.VMEM((NY, 2, TOK, 256), BF16),
            pltpu.VMEM((NY, 2, 16 * nx, cols), BF16), pltpu.VMEM((NY, 16 * nx, cols), BF16),
            pltpu.VMEM((NY, nx, 16, cols), BF16), pltpu.VMEM((NY, nx, 16, cols), BF16),
            pltpu.VMEM((NY, 16, cols), BF16), pltpu.VMEM((NY, 16, cols), BF16),
            pltpu.VMEM((NY, 16, cols), BF16), pltpu.VMEM((NY, 16, cols), BF16),
            dma((10,)), dma((10,)), dma((2, 2, rings)), dma((2, 2, rings)),
            dma((GROUP,)), dma((GROUP,)), dma((ng,)), dma((ng,)), dma((GROUP,)), dma((GROUP,)),
            dma((2, NY)), dma((2, NY)), dma((NY,)), dma((NY,)),
            dma((NY, nx)), dma((NY, nx)), dma((NY,)), dma((NY,)), pltpu.SemaphoreType.REGULAR((2,)),
        ]
        return pl.pallas_call(
            functools.partial(kernel, nz, nx),
            out_shape=jax.ShapeDtypeStruct((TOK // (2 * nx), 4 * cols), BF16),
            in_specs=[hbm] * 18,
            out_specs=vmem,
            scratch_shapes=scratch,
            compiler_params=pltpu.CompilerParams(collective_id=0, has_side_effects=True),
        )(
            asking, matching, carried, switch, source, storing, fetching,
            duality_taps, storing_taps, fetching_taps, raw, spikes, speeds, sinks.reshape(1, 2),
            gains.reshape(1, 256), jnp.swapaxes(mapping, 1, 2), jnp.asarray(starts), jnp.asarray(inner),
        )

    return jax.shard_map(
        local,
        mesh=mesh,
        in_specs=(
            P("sp", "tp"), P("sp", "tp"), P("sp", "tp"), P("sp", "tp"), P("sp", "tp"), P("sp", "tp"), P("sp", "tp"),
            P(None, "tp"), P(None, "tp"), P(None, "tp"),
            P(None, "tp", "sp"), P(None, "tp"), P(None, "tp", "sp"), P("tp"), P("tp"), P(None, "tp", "sp"),
        ),
        out_specs=P(("sp", "tp"), None),
        check_vma=False,
    )
```
